32 devices in a mesh: kv: 8 (over z, x), tp: 4 (over y, core).
Axes of the slice: x: 2, y: 2, z: 4, core: 2. Of those that a mesh axis runs over, the one named last changes fastest.
Arguments:
- tokens: bfloat16 [128, 2048], P(None, 'kv'), may hold values from -16 to 16
- norm_gain: bfloat16 [2048], P('kv'), may hold values from 0.099609375 to 1.8984375
- w_query: bfloat16 [2048, 1024], P('kv', 'tp'), may hold values from -0.125 to 0.125
- w_key: bfloat16 [2048, 1024], P('kv', 'tp'), may hold values from -0.125 to 0.125
- w_value: bfloat16 [2048, 2048], P('kv', 'tp'), may hold values from -0.125 to 0.125
- w_gate: bfloat16 [2048, 2048], P('kv', 'tp'), may hold values from -0.125 to 0.125
- w_decay: bfloat16 [2048, 1024], P('kv', 'tp'), may hold values from -0.5 to 0.5
- log_decay: float32 [128, 1024], P('kv', 'tp'), may hold values from -1.5 to 0
- state: float32 [128, 8, 128, 256], P('kv', 'tp'), may hold values from -6 to 6
- out_gain: float32 [256], replicated, may hold values from 0.1 to 1.9
- w_out: bfloat16 [2048, 2048], P('tp', 'kv'), may hold values from -0.125 to 0.125
- mixer_gain: bfloat16 [2048], P('kv'), may hold values from 0.099609375 to 1.8984375
- w_ffgate: bfloat16 [2048, 6144], P('kv', 'tp'), may hold values from -0.125 to 0.125
- w_ffup: bfloat16 [2048, 6144], P('kv', 'tp'), may hold values from -0.125 to 0.125
- w_down: bfloat16 [6144, 2048], P('tp', 'kv'), may hold values from -0.078125 to 0.078125
Outputs:
- result: bfloat16 [128, 2048], P(None, 'kv')
- new_state: float32 [128, 8, 128, 256], P('kv', 'tp')
The draws below stay inside these ranges and needn't reach their ends.
All inputs are finite; a program needn't handle non-finite values.
Results may differ from the reference program's by a relative error of at most 0.028.
Values may be sent and summed in bfloat16 or wider, within the bound.
No kernel may reach another device: no remote copies, remote signals or barrier semaphores. Data moves between devices by JAX's collectives and lax.ppermute only.
A program may use at most 64 MiB of HBM per device.

```python
import math
import jax
import jax.numpy as jnp
from jax import lax

D = 2048
HEADS = 8
DK = 128
DV = 256
FF = 6144
BATCH = 128
KW = 1024
VW = 2048
N_TP = 4


def draw_tokens(key, part):
    base = jnp.clip(jax.random.normal(jax.random.fold_in(key, 11), (BATCH, D), jnp.float32), -4.0, 4.0)
    rough = jax.random.uniform(jax.random.fold_in(key, 12), (1, D), jnp.float32, 0.5, 1.5)
    ramp = jnp.exp(jnp.linspace(0.0, math.log(6.0), D))[None, :]
    values = base * ramp * rough / 2.5
    return jnp.clip(values, -16.0, 16.0).astype(jnp.bfloat16)


def steps_of(key, shape, cuts, smallest, largest):
    def one(dim, shards_of):
        draws = jax.random.uniform(jax.random.fold_in(jax.random.fold_in(key, 6), dim), (shards_of,), jnp.float32, smallest / len(cuts), largest / len(cuts))
        return jnp.repeat(jnp.exp(draws), shape[dim] // shards_of).reshape((-1,) + (1,) * (len(shape) - dim - 1))

    loudness = one(*cuts[0])
    for cut in cuts[1:]:
        loudness = loudness * one(*cut)
    return loudness


def noise(own_key, dims, deviation, limit, shards=(), dtype=jnp.bfloat16):
    array = deviation * jax.random.normal(own_key, dims, jnp.float32)
    if shards:
        array = array * steps_of(own_key, dims, shards, -0.22, 0.18)
    return jnp.clip(array, -limit, limit).astype(dtype)


def setup_inputs(seed: int = 0) -> dict:
    arg_keys = jax.random.split(jax.random.key(seed), 16)
    tokens = draw_tokens(jax.random.fold_in(arg_keys[15], 71), 0)
    norm_gain = jnp.clip(1.0 + 0.18 * jax.random.normal(arg_keys[1], (D,), jnp.float32), 0.099609375, 1.8984375).astype(jnp.bfloat16)
    w_query = noise(arg_keys[2], (D, KW), D ** -0.5, 0.125, ((0, 8), (1, 4)))
    w_key = noise(arg_keys[3], (D, KW), D ** -0.5, 0.125, ((0, 8), (1, 4)))
    w_value = noise(arg_keys[4], (D, VW), D ** -0.5, 0.125, ((0, 8), (1, 4)))
    w_gate = noise(arg_keys[5], (D, VW), D ** -0.5, 0.125, ((0, 8), (1, 4)))
    w_decay = noise(arg_keys[6], (D, KW), (D // 16) ** -0.5, 0.5, ((0, 8), (1, 4)))
    log_decay = jnp.clip(-1.5 + 1.5 * jax.random.uniform(arg_keys[7], (BATCH, KW), jnp.float32) ** steps_of(arg_keys[7], (BATCH, KW), ((0, 8), (1, 4)), -0.2, 0.2), -1.5, 0.0)
    state = noise(arg_keys[8], (BATCH, HEADS, DK, DV), 1.0, 6.0, ((0, 8), (1, 4)), jnp.float32)
    out_gain = jnp.clip(1.0 + 0.18 * jax.random.normal(arg_keys[9], (DV,), jnp.float32), 0.1, 1.9)
    w_out = noise(arg_keys[10], (VW, D), VW ** -0.5, 0.125, ((0, 4), (1, 8)))
    mixer_gain = jnp.clip(1.0 + 0.18 * jax.random.normal(arg_keys[11], (D,), jnp.float32), 0.099609375, 1.8984375).astype(jnp.bfloat16)
    w_ffgate = noise(arg_keys[12], (D, FF), D ** -0.5, 0.125, ((0, 8), (1, 4)))
    w_ffup = noise(arg_keys[13], (D, FF), D ** -0.5, 0.125, ((0, 8), (1, 4)))
    w_down = noise(arg_keys[14], (FF, D), FF ** -0.5, 0.078125, ((0, 4), (1, 8)))
    return dict(tokens=tokens, norm_gain=norm_gain, w_query=w_query, w_key=w_key, w_value=w_value, w_gate=w_gate, w_decay=w_decay, log_decay=log_decay, state=state, out_gain=out_gain, w_out=w_out, mixer_gain=mixer_gain, w_ffgate=w_ffgate, w_ffup=w_ffup, w_down=w_down)


eps = 1e-06
gate_norm = 16.0

def group_sum(left, right, groups):
    width = left.shape[1] // groups
    total = jnp.zeros((left.shape[0], right.shape[1]), jnp.float32)
    for group in range(groups):
        part = jnp.dot(left[:, group * width:(group + 1) * width], right[group * width:(group + 1) * width], preferred_element_type=jnp.float32)
        part = lax.optimization_barrier(part.astype(jnp.bfloat16))
        total = total + part.astype(jnp.float32)
    return total

def reference(tokens, norm_gain, w_query, w_key, w_value, w_gate, w_decay, log_decay, state, out_gain, w_out, mixer_gain, w_ffgate, w_ffup, w_down):
    wide = tokens.astype(jnp.float32)
    scaled = (wide * norm_gain.astype(jnp.float32)).astype(jnp.bfloat16)
    inv = lax.rsqrt(lax.optimization_barrier(jnp.mean(wide * wide, axis=1, keepdims=True)) + eps)
    query = jnp.dot(scaled, w_query, preferred_element_type=jnp.float32) * inv
    key = jnp.dot(scaled, w_key, preferred_element_type=jnp.float32) * inv
    value = jnp.dot(scaled, w_value, preferred_element_type=jnp.float32) * inv
    gate = jnp.dot(scaled, w_gate, preferred_element_type=jnp.float32) * inv
    decay_pre = jnp.dot(scaled, w_decay, preferred_element_type=jnp.float32) * inv
    log_a = jax.nn.log_sigmoid(decay_pre) / gate_norm + log_decay
    query = query.reshape(BATCH, HEADS, DK) * DK ** (-0.5)
    key = key.reshape(BATCH, HEADS, DK)
    value = value.reshape(BATCH, HEADS, DV)
    new_state = state * jnp.exp(log_a).reshape(BATCH, HEADS, DK)[..., None] + key[..., None] * value[:, :, None, :]
    attended = jnp.einsum('bhk,bhkv->bhv', query, new_state, precision=lax.Precision.HIGHEST)
    normed = attended * lax.rsqrt(lax.optimization_barrier(jnp.mean(attended * attended, axis=2, keepdims=True)) + eps) * out_gain
    mixed = (normed.reshape(BATCH, VW) * jax.nn.silu(gate)).astype(jnp.bfloat16)
    attn_sum = group_sum(mixed, w_out, N_TP)
    middle = (wide + attn_sum).astype(jnp.bfloat16)
    wide2 = middle.astype(jnp.float32)
    scaled2 = (wide2 * mixer_gain.astype(jnp.float32)).astype(jnp.bfloat16)
    inv2 = lax.rsqrt(lax.optimization_barrier(jnp.mean(wide2 * wide2, axis=1, keepdims=True)) + eps)
    gate2 = jnp.dot(scaled2, w_ffgate, preferred_element_type=jnp.float32) * inv2
    upper = jnp.dot(scaled2, w_ffup, preferred_element_type=jnp.float32) * inv2
    hidden = (jax.nn.silu(gate2) * upper).astype(jnp.bfloat16)
    down_sum = group_sum(hidden, w_down, N_TP)
    result = (wide2 + down_sum).astype(jnp.bfloat16)
    return (result, new_state)
```

```python
import jax
import jax.numpy as jnp
from jax import lax
from jax.sharding import PartitionSpec as P

D = 2048
DK = 128
DV = 256
LANES = 128


eps = 1e-06
gate_norm = 16.0


def prepare(resid, gain):
    wide = resid.astype(jnp.float32)
    scaled = (wide * gain.astype(jnp.float32)).astype(jnp.bfloat16)
    return (scaled, jnp.sum(wide * wide, axis=1))


def split_squares(squares):
    head = squares.astype(jnp.bfloat16)
    rest = (squares - head.astype(jnp.float32)).astype(jnp.bfloat16)
    lane = lax.broadcasted_iota(jnp.int32, (squares.shape[0], LANES), 1)
    return jnp.where(lane < LANES // 2, head[:, None], rest[:, None])


def joined_squares(block):
    return block[:, :1] + block[:, LANES // 2 : LANES // 2 + 1]


def scatter_sum(array, axis):
    count = lax.axis_size(axis)
    blocks = array.reshape(count, array.shape[0] // count, array.shape[1])
    blocks = lax.all_to_all(blocks, axis, 0, 0, tiled=True)
    return jnp.sum(blocks.astype(jnp.float32), axis=0)


def gather_rows(array, axis):
    count = lax.axis_size(axis)
    copies = jnp.broadcast_to(array[None], (count,) + array.shape)
    blocks = lax.all_to_all(copies, axis, 0, 0, tiled=True)
    return blocks.reshape(count * array.shape[0], array.shape[1])


def exchange_sum(part, axis):
    count = lax.axis_size(axis)
    total = part.astype(jnp.float32)
    for step in range(1, count):
        pairs = [(i, (i + step) % count) for i in range(count)]
        total = total + lax.ppermute(part, axis, pairs).astype(jnp.float32)
    return total


def project(scaled, weights):
    return jnp.concatenate(
        [jnp.dot(scaled, weight, preferred_element_type=jnp.float32) for weight in weights], axis=1
    )


def activate(terms, sums, width):
    terms = terms * lax.rsqrt(sums / D + eps)
    return (jax.nn.silu(terms[:, :width]) * terms[:, width:]).astype(jnp.bfloat16)


def body(
    tokens,
    norm_gain,
    w_query,
    w_key,
    w_value,
    w_gate,
    w_decay,
    log_decay,
    state,
    out_gain,
    w_out,
    mixer_gain,
    w_ffgate,
    w_ffup,
    w_down,
):
    seq_dev = state.shape[0]
    heads = state.shape[1]
    key_width = w_query.shape[1]
    value_width = w_value.shape[1]
    scaled, squares = prepare(tokens, norm_gain)
    attn_weights = (w_query, w_key, w_value, w_gate, w_decay)
    part = jnp.concatenate(
        [project(scaled, attn_weights).astype(jnp.bfloat16), split_squares(squares)], axis=1
    )
    terms = scatter_sum(part, "kv")
    sums = joined_squares(terms[:, -LANES:])
    terms = terms[:, :-LANES] * lax.rsqrt(sums / D + eps)
    query = terms[:, :key_width].reshape(seq_dev, heads, DK) * DK ** (-0.5)
    keys = terms[:, key_width : 2 * key_width].reshape(seq_dev, heads, DK)
    values = terms[:, 2 * key_width : 2 * key_width + value_width].reshape(seq_dev, heads, DV)
    gate = terms[:, 2 * key_width + value_width : 2 * key_width + 2 * value_width]
    decay_pre = terms[:, 2 * key_width + 2 * value_width :]
    log_a = jax.nn.log_sigmoid(decay_pre) / gate_norm + log_decay
    new_state = (
        state * jnp.exp(log_a).reshape(seq_dev, heads, DK)[..., None]
        + keys[..., None] * values[:, :, None, :]
    )
    attended = jnp.einsum("bhk,bhkv->bhv", query, new_state, precision=lax.Precision.HIGHEST)
    normed = (
        attended * lax.rsqrt(jnp.mean(attended * attended, axis=2, keepdims=True) + eps) * out_gain
    )
    mixed = (normed.reshape(seq_dev, value_width) * jax.nn.silu(gate)).astype(jnp.bfloat16)
    partial_out = jnp.dot(gather_rows(mixed, "kv"), w_out, preferred_element_type=jnp.float32)
    attn_sum = exchange_sum(partial_out.astype(jnp.bfloat16), "tp")
    middle = (tokens.astype(jnp.float32) + attn_sum).astype(jnp.bfloat16)
    scaled2, squares2 = prepare(middle, mixer_gain)
    ff_weights = (w_ffgate, w_ffup)
    width = w_ffgate.shape[1]
    part2 = jnp.concatenate(
        [project(scaled2, ff_weights).astype(jnp.bfloat16), split_squares(squares2)], axis=1
    )
    terms2 = scatter_sum(part2, "kv")
    sums2 = joined_squares(terms2[:, -LANES:])
    hidden = gather_rows(activate(terms2[:, :-LANES], sums2, width), "kv")
    partial_down = jnp.dot(hidden, w_down, preferred_element_type=jnp.float32)
    down_total = exchange_sum(partial_down.astype(jnp.bfloat16), "tp")
    result = (middle.astype(jnp.float32) + down_total).astype(jnp.bfloat16)
    return (result, new_state)


def solution(mesh):
    return jax.shard_map(
        body,
        mesh=mesh,
        in_specs=(
            P(None, "kv"),
            P("kv"),
            P("kv", "tp"),
            P("kv", "tp"),
            P("kv", "tp"),
            P("kv", "tp"),
            P("kv", "tp"),
            P("kv", "tp"),
            P("kv", "tp", None, None),
            P(),
            P("tp", "kv"),
            P("kv"),
            P("kv", "tp"),
            P("kv", "tp"),
            P("tp", "kv"),
        ),
        out_specs=(P(None, "kv"), P("kv", "tp", None, None)),
        check_vma=False,
    )
```

```python
import functools

import jax
import jax.numpy as jnp
from jax import lax
from jax.experimental import pallas as pl
from jax.experimental.pallas import tpu as pltpu
from jax.sharding import PartitionSpec as P


D = 2048
DK = 128
DV = 256
LANES = 128
STEPS = 8


eps = 1e-06
gate_norm = 16.0


def swap_blocks(array, me, count):
    rows = array.shape[0] // count
    half = 1
    while half < count:
        view = array.reshape(count // (2 * half), 2, half * rows, array.shape[1])
        flipped = jnp.concatenate([view[:, 1:], view[:, :1]], axis=1)
        array = jnp.where((me // half) % 2 == 1, flipped, view).reshape(array.shape)
        half *= 2
    return array


def send_xor(array, sizes, masks):
    if len(sizes) == 1:
        (axis,) = sizes
        pairs = [(i, i ^ masks[0]) for i in range(sizes[axis])]
        return lax.ppermute(array, axis, pairs)
    (first, outer), (second, inner) = sizes.items()
    pairs = [
        (i * inner + j, (i ^ masks[0]) * inner + (j ^ masks[1]))
        for i in range(outer)
        for j in range(inner)
    ]
    return lax.ppermute(array, (first, second), pairs)


def wide(array):
    return array.astype(jnp.float32)


def dot(left, right):
    return jnp.dot(left, right, preferred_element_type=jnp.float32)


def split_squares(squares):
    head = squares.astype(jnp.bfloat16)
    rest = (squares - head.astype(jnp.float32)).astype(jnp.bfloat16)
    lane = lax.broadcasted_iota(jnp.int32, (squares.shape[0], LANES), 1)
    return jnp.where(lane < LANES // 2, head, rest)


def joined_squares(block):
    return block[:, :1] + block[:, LANES // 2 : LANES // 2 + 1]


VMEM = pl.BlockSpec(memory_space=pltpu.VMEM)
HBM = pl.BlockSpec(memory_space=pltpu.HBM)


def call(kernel, outs, *args, specs=None, out_specs=None, scratch=(), grant=8 << 20):
    return pl.pallas_call(
        kernel,
        out_shape=outs,
        in_specs=specs or [VMEM] * len(args),
        out_specs=out_specs or jax.tree.map(lambda _: VMEM, outs),
        scratch_shapes=list(scratch),
        compiler_params=pltpu.CompilerParams(vmem_limit_bytes=grant),
    )(*args)


def in_hbm(*arrays):
    return [pltpu.with_memory_space_constraint(array, pltpu.HBM) for array in arrays]


def shape(dims, dtype=jnp.bfloat16):
    return jax.ShapeDtypeStruct(dims, dtype)


def row(ref):
    return wide(ref[...])[None]


def block_of(ref, me, m, rows):
    return ref[pl.ds(pl.multiple_of((me ^ m) * rows, rows), rows), :]


def project_kernel(count, rows, *refs):
    loaded, (ffgate, ffup, down) = refs[:8], refs[8:11]
    pieces, (gate_out, up_out, down_out, pair_out) = refs[11 : 11 + count], refs[11 + count : 15 + count]
    staged, sems = refs[15 + count : 23 + count], refs[23 + count]
    me = lax.axis_index("kv")
    other = 1 - lax.rem(me, 2)
    half = ffgate.shape[1] // 2
    start = pl.multiple_of(other * half, half)
    loads = [pltpu.make_async_copy(w, s, sems.at[j]) for j, (w, s) in enumerate(zip(loaded, staged))]
    for load in loads:
        load.start()
    moves = [
        pltpu.make_async_copy(ffgate.at[:, pl.ds(start, half)], gate_out, sems.at[8]),
        pltpu.make_async_copy(ffup.at[:, pl.ds(start, half)], up_out, sems.at[9]),
        pltpu.make_async_copy(down.at[pl.ds(start, half)], down_out, sems.at[10]),
    ]
    for move in moves:
        move.start()
    tokens, norm_gain, mixer_gain = staged[:3]
    for load in loads[:3]:
        load.wait()
    total = tokens.shape[0]
    pair_out[:total] = tokens[...]
    pair_out[total:] = jnp.broadcast_to(row(mixer_gain), (rows, tokens.shape[1])).astype(jnp.bfloat16)
    mine = jnp.concatenate([block_of(tokens, me, m, rows) for m in range(count)], axis=0)
    mine = wide(mine)
    scaled = (mine * row(norm_gain)).astype(jnp.bfloat16)
    squares = split_squares(jnp.sum(mine * mine, axis=1, keepdims=True))
    at = 0
    for load, weight in zip(loads[3:], staged[3:]):
        load.wait()
        width = weight.shape[1]
        terms = dot(scaled, weight[...]).astype(jnp.bfloat16)
        for m in range(count):
            pieces[m][:, at : at + width] = terms[m * rows : (m + 1) * rows]
        at += width
    for m in range(count):
        pieces[m][:, at:] = squares[m * rows : (m + 1) * rows]
    for move in moves:
        move.wait()


def attend_kernel(count, key_width, steps, *refs):
    pieces, (log_decay_in, state_in, out_gain_in) = refs[:count], refs[count : count + 3]
    mixed_out, keep_out, key_out, value_out = refs[count + 3 : count + 7]
    log_decay, state, out_gain, attended, sems = refs[count + 7 :]
    rows, heads = state.shape[:2]
    some = rows // steps
    loads = [
        pltpu.make_async_copy(log_decay_in, log_decay, sems.at[0]),
        pltpu.make_async_copy(out_gain_in, out_gain, sems.at[1]),
    ] + [
        pltpu.make_async_copy(
            state_in.at[pl.ds(i * some, some)], state.at[pl.ds(i * some, some)], sems.at[2 + i]
        )
        for i in range(steps)
    ]
    for load in loads:
        load.start()
    terms = wide(pieces[0][...])
    for piece in pieces[1:]:
        terms = terms + wide(piece[...])
    inv = lax.rsqrt(joined_squares(terms[:, -LANES:]) / D + eps)
    terms = terms * inv
    value_width = heads * DV
    query = terms[:, :key_width] * DK ** (-0.5)
    keys = terms[:, key_width : 2 * key_width]
    values = terms[:, 2 * key_width : 2 * key_width + value_width]
    gate = terms[:, 2 * key_width + value_width : 2 * key_width + 2 * value_width]
    decay_pre = terms[:, 2 * key_width + 2 * value_width : 3 * key_width + 2 * value_width]
    log_sigmoid = jnp.minimum(decay_pre, 0.0) - jnp.log1p(jnp.exp(-jnp.abs(decay_pre)))
    key_out[...] = keys
    value_out[...] = values
    for load in loads[:2]:
        load.wait()
    keep = jnp.exp(log_sigmoid / gate_norm + log_decay[...])
    keep_out[...] = keep
    kept = query * keep
    columns = [kept[:, h * DK : (h + 1) * DK].T for h in range(heads)]
    for i in range(steps):
        loads[2 + i].wait()
        for b in range(i * some, (i + 1) * some):
            for h in range(heads):
                attended[b : b + 1, h * DV : (h + 1) * DV] = jnp.sum(
                    columns[h][:, b : b + 1] * state[b, h], axis=0, keepdims=True
                )
    for h in range(heads):
        lanes = slice(h * DK, (h + 1) * DK)
        outs = slice(h * DV, (h + 1) * DV)
        scores = jnp.sum(query[:, lanes] * keys[:, lanes], axis=1, keepdims=True)
        full = attended[:, outs] + scores * values[:, outs]
        scale = lax.rsqrt(jnp.mean(full * full, axis=1, keepdims=True) + eps)
        normed = full * scale * row(out_gain)
        mixed_out[:, outs] = (normed * jax.nn.silu(gate[:, outs])).astype(jnp.bfloat16)


def rows_kernel(count, *refs):
    blocks, (first, second, out) = refs[:count], refs[count:]
    left = jnp.concatenate([block[...] for block in blocks], axis=0)
    depth, model = second.shape
    start = lax.rem(lax.axis_index("kv"), 2) * depth if first.shape[0] > depth else 0
    kept = first[pl.ds(pl.multiple_of(start, depth), depth)] if first.shape[0] > depth else first[...]
    out[:, :model] = dot(left, kept).astype(jnp.bfloat16)
    out[:, model:] = dot(left, second[...]).astype(jnp.bfloat16)


def middle_kernel(n_even, n_odd, *refs):
    evens, odds = refs[:n_even], refs[n_even : n_even + n_odd]
    tokens, pair, mixer_gain, ffgate, ffup, gate_pair, up_pair = refs[n_even + n_odd :][:7]
    middle_out, *pieces = refs[n_even + n_odd + 7 :]
    me = lax.axis_index("kv")
    batch, model = tokens.shape
    half = gate_pair.shape[1]
    count = 2 * len(pieces)
    rows = batch // count
    even = sum(wide(ref[...]) for ref in evens)
    odd = sum(wide(ref[...]) for ref in odds)

    def stream(stay, first, second):
        blocks = []
        for m in range(count):
            source = first if m % 2 == 0 else second
            blocks.append(
                wide(block_of(stay, me, m, rows)) + source[m // 2 * rows : (m // 2 + 1) * rows]
            )
        return wide(jnp.concatenate(blocks, axis=0).astype(jnp.bfloat16))

    own = stream(tokens, even[:, :model], odd[:, model:])
    other = stream(pair, even[:, model:], odd[:, :model])
    middle_out[...] = own.astype(jnp.bfloat16)
    own2 = (own * row(mixer_gain)).astype(jnp.bfloat16)
    other2 = (other * wide(pair[batch : batch + 1])).astype(jnp.bfloat16)
    squares = jnp.sum(own * own, axis=1, keepdims=True) + jnp.sum(other * other, axis=1, keepdims=True)
    squares = split_squares(squares)
    kept = pl.ds(pl.multiple_of(lax.rem(me, 2) * half, half), half)
    gate = (dot(own2, ffgate[:, kept]) + dot(other2, gate_pair[...])).astype(jnp.bfloat16)
    upper = (dot(own2, ffup[:, kept]) + dot(other2, up_pair[...])).astype(jnp.bfloat16)
    for i, piece in enumerate(pieces):
        part = slice(2 * i * rows, 2 * (i + 1) * rows)
        piece[:, :half] = gate[part]
        piece[:, half : 2 * half] = upper[part]
        piece[:, 2 * half :] = squares[part]


def hidden_kernel(count, *refs):
    pieces, out = refs[:count], refs[count]
    half = out.shape[1]
    terms = sum(wide(piece[...]) for piece in pieces)
    inv = lax.rsqrt(joined_squares(terms[:, 2 * half :]) / D + eps)
    hidden = jax.nn.silu(terms[:, :half] * inv) * (terms[:, half : 2 * half] * inv)
    out[...] = hidden.astype(jnp.bfloat16)


def body(
    tokens,
    norm_gain,
    w_query,
    w_key,
    w_value,
    w_gate,
    w_decay,
    log_decay,
    state,
    out_gain,
    w_out,
    mixer_gain,
    w_ffgate,
    w_ffup,
    w_down,
):
    n_kv = lax.axis_size("kv")
    n_tp = lax.axis_size("tp")
    kv, tp, both = {"kv": n_kv}, {"tp": n_tp}, {"kv": n_kv, "tp": n_tp}
    me = lax.axis_index("kv")
    rows = state.shape[0]
    heads = state.shape[1]
    key_width = w_query.shape[1]
    value_width = w_value.shape[1]
    model = tokens.shape[1]
    half = w_ffgate.shape[1] // 2

    batch = tokens.shape[0]
    attn_weights = (w_query, w_key, w_value, w_gate, w_decay)
    total_width = sum(w.shape[1] for w in attn_weights) + LANES
    loaded = (tokens, norm_gain, mixer_gain) + attn_weights
    made = call(
        functools.partial(project_kernel, n_kv, rows),
        [shape((rows, total_width))] * n_kv
        + [shape((model, half))] * 2
        + [shape((half, model)), shape((batch + rows, model))],
        *in_hbm(*loaded, w_ffgate, w_ffup, w_down),
        specs=[HBM] * 11,
        out_specs=[VMEM] * (n_kv + 4),
        scratch=[pltpu.VMEM(w.shape, w.dtype) for w in loaded]
        + [pltpu.SemaphoreType.DMA((11,))],
    )
    pieces, (gate_sent, up_sent, down_sent, pair_sent) = made[:n_kv], made[n_kv:]
    gate_pair = send_xor(gate_sent, kv, (1,))
    order = [m for m in range(2, n_kv, 2)][::-1] + [m for m in range(1, n_kv, 2)][::-1]
    came = {}
    for m in order:
        came[m] = send_xor(pieces[m], kv, (m,))
    out_pair = send_xor(w_out, kv, (1,))
    up_pair = send_xor(up_sent, kv, (1,))
    pair = send_xor(pair_sent, kv, (1,))
    down_pair = send_xor(down_sent, kv, (1,))

    mixed, keep, keys, values = call(
        functools.partial(attend_kernel, n_kv, key_width, STEPS),
        [shape((rows, value_width))]
        + [shape((rows, w), jnp.float32) for w in (key_width, key_width, value_width)],
        pieces[0],
        *[came[m] for m in order],
        *in_hbm(log_decay, state, out_gain),
        specs=[VMEM] * n_kv + [HBM] * 3,
        scratch=[
            pltpu.VMEM(log_decay.shape, jnp.float32),
            pltpu.VMEM(state.shape, jnp.float32),
            pltpu.VMEM(out_gain.shape, jnp.float32),
            pltpu.VMEM((rows, value_width), jnp.float32),
            pltpu.SemaphoreType.DMA((2 + STEPS,)),
        ],
        grant=12 << 20,
    )

    evens = list(range(2, n_kv, 2))
    blocks = {}
    for m in evens[::-1]:
        blocks[m] = send_xor(mixed, kv, (m,))
    new_state = (
        state * keep.reshape(rows, heads, DK)[..., None]
        + keys.reshape(rows, heads, DK)[..., None]
        * values.reshape(rows, heads, DV)[:, :, None, :]
    )
    chip = call(
        functools.partial(rows_kernel, n_kv // 2),
        shape((n_kv // 2 * rows, 2 * model)),
        mixed,
        *[blocks[m] for m in evens],
        w_out,
        out_pair,
    )
    chip_core = send_xor(chip, tp, (1,))
    sent = (wide(chip) + wide(chip_core)).astype(jnp.bfloat16)
    even, odd = [chip, chip_core], []
    for m in range(0, n_tp, 2)[::-1]:
        odd.append(send_xor(sent, both, (1, m)))
        if m:
            even.append(send_xor(sent, both, (0, m)))

    middle, *parts = call(
        functools.partial(middle_kernel, len(even), len(odd)),
        [shape((batch, model))] + [shape((2 * rows, 2 * half + LANES))] * (n_kv // 2),
        *even,
        *odd,
        tokens,
        pair,
        mixer_gain,
        w_ffgate,
        w_ffup,
        gate_pair,
        up_pair,
    )
    terms2 = [parts[0]]
    for m in evens[::-1]:
        terms2.append(send_xor(parts[m // 2], kv, (m,)))
    hidden = call(functools.partial(hidden_kernel, n_kv // 2), shape((2 * rows, half)), *terms2)

    blocks = {}
    for m in evens[::-1]:
        blocks[m] = send_xor(hidden, kv, (m,))
    down = call(
        functools.partial(rows_kernel, n_kv // 2),
        shape((batch, 2 * model)),
        hidden,
        *[blocks[m] for m in evens],
        w_down,
        down_pair,
    )
    down = wide(down) + wide(send_xor(down, tp, (1,)))
    own, other = down[:, :model], down[:, model:].astype(jnp.bfloat16)
    sent = own.astype(jnp.bfloat16)
    crossed = 0.0
    for m in range(0, n_tp, 2)[::-1]:
        crossed = crossed + wide(send_xor(other, both, (1, m)))
        if m:
            own = own + wide(send_xor(sent, both, (0, m)))
    crossed = crossed.reshape(n_kv // 2, 2, rows, model)
    crossed = jnp.concatenate([crossed[:, 1:], crossed[:, :1]], axis=1).reshape(own.shape)
    result = (wide(middle) + own + crossed).astype(jnp.bfloat16)
    return (swap_blocks(result, me, n_kv), new_state)


def solution(mesh):
    return jax.shard_map(
        body,
        mesh=mesh,
        in_specs=(
            P(None, "kv"),
            P("kv"),
            P("kv", "tp"),
            P("kv", "tp"),
            P("kv", "tp"),
            P("kv", "tp"),
            P("kv", "tp"),
            P("kv", "tp"),
            P("kv", "tp", None, None),
            P(),
            P("tp", "kv"),
            P("kv"),
            P("kv", "tp"),
            P("kv", "tp"),
            P("tp", "kv"),
        ),
        out_specs=(P(None, "kv"), P("kv", "tp", None, None)),
        check_vma=False,
    )
```

```python
import functools

import jax
import jax.numpy as jnp
from jax import lax
from jax.experimental import pallas as pl
from jax.experimental.pallas import tpu as pltpu
from jax.sharding import PartitionSpec as P


D = 2048
DK = 128
DV = 256
LANES = 128
STEPS = 8
SCATTER = (1, 4, 5, 3, 6, 2)
NEAR = (6, 4, 2)
FF_GATE = (6, 4, 2)
FF_UP = (6, 4, 2)
LATE = 4
HIDDEN = (6, 4, 2)


eps = 1e-06
gate_norm = 16.0


def swap_blocks(array, me, count):
    rows = array.shape[0] // count
    half = 1
    while half < count:
        view = array.reshape(count // (2 * half), 2, half * rows, array.shape[1])
        flipped = jnp.concatenate([view[:, 1:], view[:, :1]], axis=1)
        array = jnp.where((me // half) % 2 == 1, flipped, view).reshape(array.shape)
        half *= 2
    return array


def send_xor(array, sizes, masks):
    if len(sizes) == 1:
        (axis,) = sizes
        pairs = [(i, i ^ masks[0]) for i in range(sizes[axis])]
        return lax.ppermute(array, axis, pairs)
    (first, outer), (second, inner) = sizes.items()
    pairs = [
        (i * inner + j, (i ^ masks[0]) * inner + (j ^ masks[1]))
        for i in range(outer)
        for j in range(inner)
    ]
    return lax.ppermute(array, (first, second), pairs)


def wide(array):
    return array.astype(jnp.float32)


def dot(left, right):
    return jnp.dot(left, right, preferred_element_type=jnp.float32)


def split_squares(squares):
    head = squares.astype(jnp.bfloat16)
    rest = (squares - head.astype(jnp.float32)).astype(jnp.bfloat16)
    lane = lax.broadcasted_iota(jnp.int32, (squares.shape[0], LANES), 1)
    return jnp.where(lane < LANES // 2, head, rest)


def joined_squares(block):
    return block[:, :1] + block[:, LANES // 2 : LANES // 2 + 1]


VMEM = pl.BlockSpec(memory_space=pltpu.VMEM)
HBM = pl.BlockSpec(memory_space=pltpu.HBM)


def call(kernel, outs, *args, specs=None, out_specs=None, scratch=(), grant=8 << 20):
    return pl.pallas_call(
        kernel,
        out_shape=outs,
        in_specs=specs or [VMEM] * len(args),
        out_specs=out_specs or jax.tree.map(lambda _: VMEM, outs),
        scratch_shapes=list(scratch),
        compiler_params=pltpu.CompilerParams(vmem_limit_bytes=grant),
    )(*args)


def in_hbm(*arrays):
    return [pltpu.with_memory_space_constraint(array, pltpu.HBM) for array in arrays]


def shape(dims, dtype=jnp.bfloat16):
    return jax.ShapeDtypeStruct(dims, dtype)


def row(ref):
    return wide(ref[...])[None]


def block_of(ref, me, m, rows):
    return ref[pl.ds(pl.multiple_of((me ^ m) * rows, rows), rows), :]


def place_of(m, count, rows):
    return (1, slice(rows, 2 * rows)) if m == count - 1 else (m, slice(0, rows))


def relay_kernel(piece, came, out):
    rows = piece.shape[0]
    terms = wide(piece[...]) + wide(came[rows:])
    out[:, :-LANES] = terms[:, :-LANES].astype(jnp.bfloat16)
    out[:, -LANES:] = split_squares(joined_squares(terms[:, -LANES:]))


def project_kernel(count, rows, *refs):
    loaded, (ffgate, ffup, down) = refs[:8], refs[8:11]
    pieces, (early_out, late_out, down_out, pair_out) = refs[11 : 10 + count], refs[10 + count : 14 + count]
    staged, sems = refs[14 + count : 22 + count], refs[22 + count]
    me = lax.axis_index("kv")
    other = 1 - lax.rem(me, 2)
    half = ffgate.shape[1] // 2
    start = pl.multiple_of(other * half, LANES)
    first = half - late_out.shape[1]
    loads = [pltpu.make_async_copy(w, s, sems.at[j]) for j, (w, s) in enumerate(zip(loaded, staged))]
    for load in loads:
        load.start()
    moves = [
        pltpu.make_async_copy(ffgate.at[:, pl.ds(start, half)], early_out.at[:, :half], sems.at[8]),
        pltpu.make_async_copy(ffup.at[:, pl.ds(start, first)], early_out.at[:, half:], sems.at[9]),
        pltpu.make_async_copy(ffup.at[:, pl.ds(start + first, half - first)], late_out, sems.at[10]),
        pltpu.make_async_copy(down.at[pl.ds(start, half)], down_out, sems.at[11]),
    ]
    for move in moves:
        move.start()
    tokens, norm_gain, mixer_gain = staged[:3]
    for load in loads[:3]:
        load.wait()
    mine = jnp.concatenate([block_of(tokens, me, m, rows) for m in range(count)], axis=0)
    total, model = tokens.shape
    pair_out[:total] = mine
    pair_out[total:] = jnp.broadcast_to(row(mixer_gain), (rows, model)).astype(jnp.bfloat16)
    mine = wide(mine)
    scaled = (mine * row(norm_gain)).astype(jnp.bfloat16)
    squares = split_squares(jnp.sum(mine * mine, axis=1, keepdims=True))
    at = 0
    for load, weight in zip(loads[3:], staged[3:]):
        load.wait()
        width = weight.shape[1]
        terms = dot(scaled, weight[...]).astype(jnp.bfloat16)
        for m in range(count):
            block, top = place_of(m, count, rows)
            pieces[block][top, at : at + width] = terms[m * rows : (m + 1) * rows]
        at += width
    for m in range(count):
        block, top = place_of(m, count, rows)
        pieces[block][top, at:] = squares[m * rows : (m + 1) * rows]
    for move in moves:
        move.wait()


def load_kernel(*refs):
    loads = [pltpu.make_async_copy(refs[j], refs[3 + j], refs[6].at[j]) for j in range(3)]
    for load in loads:
        load.start()
    for load in loads:
        load.wait()


def update_kernel(steps, state, keep, keys, values, out, fresh, sems):
    rows, heads = state.shape[:2]
    some = rows // steps
    keep_columns = [keep[:, h * DK : (h + 1) * DK].T for h in range(heads)]
    key_columns = [keys[:, h * DK : (h + 1) * DK].T for h in range(heads)]
    stores = []
    for i in range(steps):
        for b in range(i * some, (i + 1) * some):
            for h in range(heads):
                fresh[b, h] = (
                    keep_columns[h][:, b : b + 1] * state[b, h]
                    + key_columns[h][:, b : b + 1] * values[b : b + 1, h * DV : (h + 1) * DV]
                )
        part = pl.ds(i * some, some)
        stores.append(pltpu.make_async_copy(fresh.at[part], out.at[part], sems.at[i]))
        stores[-1].start()
    for store in stores:
        store.wait()


def attend_kernel(count, key_width, *refs):
    pieces, (log_decay, state, out_gain) = refs[:count], refs[count : count + 3]
    mixed_out, keep_out, key_out, value_out, attended = refs[count + 3 :]
    rows, heads = state.shape[:2]
    terms = wide(pieces[0][...])
    for piece in pieces[1:]:
        terms = terms + wide(piece[:rows])
    inv = lax.rsqrt(joined_squares(terms[:, -LANES:]) / D + eps)
    terms = terms * inv
    value_width = heads * DV
    query = terms[:, :key_width] * DK ** (-0.5)
    keys = terms[:, key_width : 2 * key_width]
    values = terms[:, 2 * key_width : 2 * key_width + value_width]
    gate = terms[:, 2 * key_width + value_width : 2 * key_width + 2 * value_width]
    decay_pre = terms[:, 2 * key_width + 2 * value_width : 3 * key_width + 2 * value_width]
    log_sigmoid = jnp.minimum(decay_pre, 0.0) - jnp.log1p(jnp.exp(-jnp.abs(decay_pre)))
    key_out[...] = keys
    value_out[...] = values
    keep = jnp.exp(log_sigmoid / gate_norm + log_decay[...])
    keep_out[...] = keep
    kept = query * keep
    columns = [kept[:, h * DK : (h + 1) * DK].T for h in range(heads)]
    for b in range(rows):
        for h in range(heads):
            attended[b : b + 1, h * DV : (h + 1) * DV] = jnp.sum(
                columns[h][:, b : b + 1] * state[b, h], axis=0, keepdims=True
            )
    for h in range(heads):
        lanes = slice(h * DK, (h + 1) * DK)
        outs = slice(h * DV, (h + 1) * DV)
        scores = jnp.sum(query[:, lanes] * keys[:, lanes], axis=1, keepdims=True)
        full = attended[:, outs] + scores * values[:, outs]
        scale = lax.rsqrt(jnp.mean(full * full, axis=1, keepdims=True) + eps)
        normed = full * scale * row(out_gain)
        mixed_out[:, outs] = (normed * jax.nn.silu(gate[:, outs])).astype(jnp.bfloat16)


def rows_kernel(count, *refs):
    blocks, (first, second, out) = refs[:count], refs[count:]
    left = jnp.concatenate([block[...] for block in blocks], axis=0)
    depth, model = second.shape
    start = lax.rem(lax.axis_index("kv"), 2) * depth if first.shape[0] > depth else 0
    kept = first[pl.ds(pl.multiple_of(start, depth), depth)] if first.shape[0] > depth else first[...]
    out[:, :model] = dot(left, kept).astype(jnp.bfloat16)
    out[:, model:] = dot(left, second[...]).astype(jnp.bfloat16)


def middle_kernel(n_even, n_odd, *refs):
    evens, odds = refs[:n_even], refs[n_even : n_even + n_odd]
    tokens, pair, mixer_gain, ffgate, sent = refs[n_even + n_odd :][:5]
    middle_out, own_out, other_out, *pieces = refs[n_even + n_odd + 5 :]
    me = lax.axis_index("kv")
    batch, model = tokens.shape
    half = ffgate.shape[1] // 2
    count = 2 * len(pieces)
    rows = batch // count
    even = sum(wide(ref[...]) for ref in evens)
    odd = sum(wide(ref[...]) for ref in odds)

    def pair_block(m):
        return pair[(m ^ 1) * rows : ((m ^ 1) + 1) * rows]

    def stream(stay, first, second):
        blocks = []
        for m in range(count):
            source = first if m % 2 == 0 else second
            blocks.append(wide(stay(m)) + source[m // 2 * rows : (m // 2 + 1) * rows])
        return wide(jnp.concatenate(blocks, axis=0).astype(jnp.bfloat16))

    own = stream(lambda m: block_of(tokens, me, m, rows), even[:, :model], odd[:, model:])
    other = stream(pair_block, even[:, model:], odd[:, :model])
    middle_out[...] = own.astype(jnp.bfloat16)
    own2 = (own * row(mixer_gain)).astype(jnp.bfloat16)
    other2 = (other * wide(pair[batch : batch + 1])).astype(jnp.bfloat16)
    own_out[...] = own2
    other_out[...] = other2
    squares = jnp.sum(own * own, axis=1, keepdims=True) + jnp.sum(other * other, axis=1, keepdims=True)
    squares = split_squares(squares)
    kept = pl.ds(pl.multiple_of(lax.rem(me, 2) * half, half), half)
    gate = (dot(own2, ffgate[:, kept]) + dot(other2, sent[:, :half])).astype(jnp.bfloat16)
    for i, piece in enumerate(pieces):
        part = slice(2 * i * rows, 2 * (i + 1) * rows)
        piece[:, :half] = gate[part]
        piece[:, half:] = squares[part]


def upper_kernel(own2, other2, ffup, early, late, *pieces):
    half = ffup.shape[1] // 2
    first = half - late.shape[1]
    rows = own2.shape[0] // len(pieces)
    kept = pl.ds(pl.multiple_of(lax.rem(lax.axis_index("kv"), 2) * half, half), half)
    upper = dot(own2[...], ffup[:, kept])
    for columns, weight in ((slice(0, first), early[:, half:]), (slice(first, half), late[...])):
        part = (upper[:, columns] + dot(other2[...], weight)).astype(jnp.bfloat16)
        for i, piece in enumerate(pieces):
            piece[:, columns] = part[i * rows : (i + 1) * rows]


def hidden_kernel(count, *refs):
    gates, uppers, out = refs[:count], refs[count : 2 * count], refs[2 * count]
    half = out.shape[1]
    gate = sum(wide(piece[...]) for piece in gates)
    upper = sum(wide(piece[...]) for piece in uppers)
    inv = lax.rsqrt(joined_squares(gate[:, half:]) / D + eps)
    hidden = jax.nn.silu(gate[:, :half] * inv) * (upper * inv)
    out[...] = hidden.astype(jnp.bfloat16)


def body(
    tokens,
    norm_gain,
    w_query,
    w_key,
    w_value,
    w_gate,
    w_decay,
    log_decay,
    state,
    out_gain,
    w_out,
    mixer_gain,
    w_ffgate,
    w_ffup,
    w_down,
):
    n_kv = lax.axis_size("kv")
    n_tp = lax.axis_size("tp")
    kv, tp, both = {"kv": n_kv}, {"tp": n_tp}, {"kv": n_kv, "tp": n_tp}
    me = lax.axis_index("kv")
    rows = state.shape[0]
    key_width = w_query.shape[1]
    value_width = w_value.shape[1]
    model = tokens.shape[1]
    half = w_ffgate.shape[1] // 2

    batch = tokens.shape[0]
    attn_weights = (w_query, w_key, w_value, w_gate, w_decay)
    total_width = sum(w.shape[1] for w in attn_weights) + LANES
    late = half * LATE // (6 * LANES) * LANES
    loaded = (tokens, norm_gain, mixer_gain) + attn_weights
    made = call(
        functools.partial(project_kernel, n_kv, rows),
        [shape((rows + (m == 1) * rows, total_width)) for m in range(n_kv - 1)]
        + [shape((model, half + half - late)), shape((model, late))]
        + [shape((half, model)), shape((batch + rows, model))],
        *in_hbm(*loaded, w_ffgate, w_ffup, w_down),
        specs=[HBM] * 11,
        out_specs=[VMEM] * (n_kv + 3),
        scratch=[pltpu.VMEM(w.shape, w.dtype) for w in loaded]
        + [pltpu.SemaphoreType.DMA((12,))],
    )
    pieces, (early_sent, late_sent, down_sent, pair_sent) = made[: n_kv - 1], made[n_kv - 1 :]
    order = order_of(SCATTER, range(1, n_kv - 1))
    came = {}
    came[1] = send_xor(pieces[1], kv, (1,))
    relayed = call(relay_kernel, shape((rows, total_width)), pieces[n_kv - 2], came[1])
    for m in order[1:]:
        came[m] = send_xor(relayed if m == n_kv - 2 else pieces[m], kv, (m,))
    out_pair = send_xor(w_out, kv, (1,))
    early_pair = send_xor(early_sent, kv, (1,))
    pair = send_xor(pair_sent, kv, (1,))
    late_pair = send_xor(late_sent, kv, (1,))
    down_pair = send_xor(down_sent, kv, (1,))
    state_near, log_decay_near, out_gain_near = call(
        load_kernel,
        [pltpu.VMEM(x.shape, x.dtype) for x in (state, log_decay, out_gain)],
        *in_hbm(state, log_decay, out_gain),
        specs=[HBM] * 3,
        scratch=[pltpu.SemaphoreType.DMA((3,))],
    )

    mixed, keep, keys, values = call(
        functools.partial(attend_kernel, n_kv - 1, key_width),
        [shape((rows, value_width))]
        + [shape((rows, w), jnp.float32) for w in (key_width, key_width, value_width)],
        pieces[0],
        *[came[m] for m in order],
        log_decay_near,
        state_near,
        out_gain_near,
        scratch=[pltpu.VMEM((rows, value_width), jnp.float32)],
    )

    evens = list(range(2, n_kv, 2))
    blocks = {}
    for m in order_of(NEAR, evens):
        blocks[m] = send_xor(mixed, kv, (m,))
    new_state = call(
        functools.partial(update_kernel, STEPS),
        shape(state.shape, jnp.float32),
        state_near,
        keep,
        keys,
        values,
        out_specs=HBM,
        scratch=[
            pltpu.VMEM(state.shape, jnp.float32),
            pltpu.SemaphoreType.DMA((STEPS,)),
        ],
    )
    chip = call(
        functools.partial(rows_kernel, n_kv // 2),
        shape((n_kv // 2 * rows, 2 * model)),
        mixed,
        *[blocks[m] for m in evens],
        w_out,
        out_pair,
    )
    chip_core = send_xor(chip, tp, (1,))
    sent = (wide(chip) + wide(chip_core)).astype(jnp.bfloat16)
    even, odd = [chip, chip_core], []
    for m in range(0, n_tp, 2)[::-1]:
        odd.append(send_xor(sent, both, (1, m)))
        if m:
            even.append(send_xor(sent, both, (0, m)))

    middle, own2, other2, *gates = call(
        functools.partial(middle_kernel, len(even), len(odd)),
        [shape((batch, model))] * 3 + [shape((2 * rows, half + LANES))] * (n_kv // 2),
        *even,
        *odd,
        tokens,
        pair,
        mixer_gain,
        w_ffgate,
        early_pair,
    )
    terms2 = [gates[0]]
    for m in order_of(FF_GATE, evens):
        terms2.append(send_xor(gates[m // 2], kv, (m,)))
    uppers = call(
        upper_kernel,
        [shape((2 * rows, half))] * (n_kv // 2),
        own2,
        other2,
        w_ffup,
        early_pair,
        late_pair,
    )
    terms2.append(uppers[0])
    for m in order_of(FF_UP, evens):
        terms2.append(send_xor(uppers[m // 2], kv, (m,)))
    hidden = call(functools.partial(hidden_kernel, n_kv // 2), shape((2 * rows, half)), *terms2)

    blocks = {}
    for m in order_of(HIDDEN, evens):
        blocks[m] = send_xor(hidden, kv, (m,))
    down = call(
        functools.partial(rows_kernel, n_kv // 2),
        shape((batch, 2 * model)),
        hidden,
        *[blocks[m] for m in evens],
        w_down,
        down_pair,
    )
    down = wide(down) + wide(send_xor(down, tp, (1,)))
    own, other = down[:, :model], down[:, model:].astype(jnp.bfloat16)
    sent = own.astype(jnp.bfloat16)
    crossed = 0.0
    for m in range(0, n_tp, 2)[::-1]:
        crossed = crossed + wide(send_xor(other, both, (1, m)))
        if m:
            own = own + wide(send_xor(sent, both, (0, m)))
    crossed = crossed.reshape(n_kv // 2, 2, rows, model)
    crossed = jnp.concatenate([crossed[:, 1:], crossed[:, :1]], axis=1).reshape(own.shape)
    result = (wide(middle) + own + crossed).astype(jnp.bfloat16)
    return (swap_blocks(result, me, n_kv), new_state)


def order_of(wanted, masks):
    if sorted(wanted) == sorted(masks):
        return list(wanted)
    return [m for m in masks if m == 1] + [m for m in masks if m != 1][::-1]


def solution(mesh):
    return jax.shard_map(
        body,
        mesh=mesh,
        in_specs=(
            P(None, "kv"),
            P("kv"),
            P("kv", "tp"),
            P("kv", "tp"),
            P("kv", "tp"),
            P("kv", "tp"),
            P("kv", "tp"),
            P("kv", "tp"),
            P("kv", "tp", None, None),
            P(),
            P("tp", "kv"),
            P("kv"),
            P("kv", "tp"),
            P("kv", "tp"),
            P("tp", "kv"),
        ),
        out_specs=(P(None, "kv"), P("kv", "tp", None, None)),
        check_vma=False,
    )
```

```python
import functools

import jax
import jax.numpy as jnp
from jax import lax
from jax.experimental import pallas as pl
from jax.experimental.pallas import tpu as pltpu
from jax.sharding import PartitionSpec as P


D = 2048
DK = 128
DV = 256
LANES = 128
TILE = 8
STEPS = 8
SCATTER = (1, 3, 4, 5, 6, 2)
NEAR = (6, 4, 2)
FF_GATE = (6, 4, 2)
FF_UP = (6, 4, 2)
LATE = 4
HIDDEN = (6, 4, 2)


eps = 1e-06
gate_norm = 16.0


def swap_blocks(array, me, count):
    rows = array.shape[0] // count
    half = 1
    while half < count:
        view = array.reshape(count // (2 * half), 2, half * rows, array.shape[1])
        flipped = jnp.concatenate([view[:, 1:], view[:, :1]], axis=1)
        array = jnp.where((me // half) % 2 == 1, flipped, view).reshape(array.shape)
        half *= 2
    return array


def send_xor(array, sizes, masks):
    if len(sizes) == 1:
        (axis,) = sizes
        pairs = [(i, i ^ masks[0]) for i in range(sizes[axis])]
        return lax.ppermute(array, axis, pairs)
    (first, outer), (second, inner) = sizes.items()
    pairs = [
        (i * inner + j, (i ^ masks[0]) * inner + (j ^ masks[1]))
        for i in range(outer)
        for j in range(inner)
    ]
    return lax.ppermute(array, (first, second), pairs)


def wide(array):
    return array.astype(jnp.float32)


def dot(left, right):
    return jnp.dot(left, right, preferred_element_type=jnp.float32)


def split_squares(squares):
    head = squares.astype(jnp.bfloat16)
    rest = (squares - head.astype(jnp.float32)).astype(jnp.bfloat16)
    lane = lax.broadcasted_iota(jnp.int32, (squares.shape[0], LANES), 1)
    return jnp.where(lane < LANES // 2, head, rest)


def joined_squares(block):
    return block[:, :1] + block[:, LANES // 2 : LANES // 2 + 1]


VMEM = pl.BlockSpec(memory_space=pltpu.VMEM)
HBM = pl.BlockSpec(memory_space=pltpu.HBM)


def call(kernel, outs, *args, specs=None, out_specs=None, scratch=(), grant=8 << 20):
    return pl.pallas_call(
        kernel,
        out_shape=outs,
        in_specs=specs or [VMEM] * len(args),
        out_specs=out_specs or jax.tree.map(lambda _: VMEM, outs),
        scratch_shapes=list(scratch),
        compiler_params=pltpu.CompilerParams(vmem_limit_bytes=grant),
    )(*args)


def in_hbm(*arrays):
    return [pltpu.with_memory_space_constraint(array, pltpu.HBM) for array in arrays]


def shape(dims, dtype=jnp.bfloat16):
    return jax.ShapeDtypeStruct(dims, dtype)


def row(ref):
    return wide(ref[...])[None]


def block_of(ref, me, m, rows):
    return ref[pl.ds(pl.multiple_of((me ^ m) * rows, rows), rows), :]


def place_of(m, count, rows):
    return (1, slice(rows, 2 * rows)) if m == count - 1 else (m, slice(0, rows))


def relay_kernel(piece, came, out):
    rows = piece.shape[0]
    terms = wide(piece[...]) + wide(came[rows:])
    out[:, :-LANES] = terms[:, :-LANES].astype(jnp.bfloat16)
    out[:, -LANES:] = split_squares(joined_squares(terms[:, -LANES:]))


def project_kernel(count, rows, *refs):
    loaded, (ffgate, ffup, down) = refs[:8], refs[8:11]
    pieces, (early_out, late_out, down_out, pair_out) = refs[11 : 10 + count], refs[10 + count : 14 + count]
    staged, sems = refs[14 + count : 22 + count], refs[22 + count]
    me = lax.axis_index("kv")
    other = 1 - lax.rem(me, 2)
    half = ffgate.shape[1] // 2
    start = pl.multiple_of(other * half, LANES)
    first = half - late_out.shape[1]
    loads = [pltpu.make_async_copy(w, s, sems.at[j]) for j, (w, s) in enumerate(zip(loaded, staged))]
    for load in loads:
        load.start()
    moves = [
        pltpu.make_async_copy(ffgate.at[:, pl.ds(start, half)], early_out.at[:, :half], sems.at[8]),
        pltpu.make_async_copy(ffup.at[:, pl.ds(start, first)], early_out.at[:, half:], sems.at[9]),
        pltpu.make_async_copy(ffup.at[:, pl.ds(start + first, half - first)], late_out, sems.at[10]),
        pltpu.make_async_copy(down.at[pl.ds(start, half)], down_out, sems.at[11]),
    ]
    for move in moves:
        move.start()
    tokens, norm_gain, mixer_gain = staged[:3]
    for load in loads[:3]:
        load.wait()
    mine = jnp.concatenate([block_of(tokens, me, m, rows) for m in range(count)], axis=0)
    total, model = tokens.shape
    pair_out[:total] = mine
    pair_out[total:] = jnp.broadcast_to(row(mixer_gain), (rows, model)).astype(jnp.bfloat16)
    mine = wide(mine)
    scaled = (mine * row(norm_gain)).astype(jnp.bfloat16)
    squares = split_squares(jnp.sum(mine * mine, axis=1, keepdims=True))
    at = 0
    for load, weight in zip(loads[3:], staged[3:]):
        load.wait()
        width = weight.shape[1]
        terms = dot(scaled, weight[...]).astype(jnp.bfloat16)
        for m in range(count):
            block, top = place_of(m, count, rows)
            pieces[block][top, at : at + width] = terms[m * rows : (m + 1) * rows]
        at += width
    for m in range(count):
        block, top = place_of(m, count, rows)
        pieces[block][top, at:] = squares[m * rows : (m + 1) * rows]
    for move in moves:
        move.wait()


def load_kernel(*refs):
    loads = [pltpu.make_async_copy(refs[j], refs[3 + j], refs[6].at[j]) for j in range(3)]
    for load in loads:
        load.start()
    for load in loads:
        load.wait()


def update_kernel(steps, state, keep, keys, values, out, fresh, sems):
    rows, heads = state.shape[:2]
    some = rows // steps
    keep_columns = [keep[:, h * DK : (h + 1) * DK].T for h in range(heads)]
    key_columns = [keys[:, h * DK : (h + 1) * DK].T for h in range(heads)]
    stores = []
    for i in range(steps):
        for b in range(i * some, (i + 1) * some):
            for h in range(heads):
                fresh[b, h] = (
                    keep_columns[h][:, b : b + 1] * state[b, h]
                    + key_columns[h][:, b : b + 1] * values[b : b + 1, h * DV : (h + 1) * DV]
                )
        part = pl.ds(i * some, some)
        stores.append(pltpu.make_async_copy(fresh.at[part], out.at[part], sems.at[i]))
        stores[-1].start()
    for store in stores:
        store.wait()


def attend_kernel(count, key_width, *refs):
    pieces, (log_decay, state, out_gain) = refs[:count], refs[count : count + 3]
    mixed_out, keep_out, key_out, value_out, attended = refs[count + 3 :]
    rows, heads = state.shape[:2]
    terms = wide(pieces[0][...])
    for piece in pieces[1:]:
        terms = terms + wide(piece[:rows])
    inv = lax.rsqrt(joined_squares(terms[:, -LANES:]) / D + eps)
    terms = terms * inv
    value_width = heads * DV
    query = terms[:, :key_width] * DK ** (-0.5)
    keys = terms[:, key_width : 2 * key_width]
    values = terms[:, 2 * key_width : 2 * key_width + value_width]
    gate = terms[:, 2 * key_width + value_width : 2 * key_width + 2 * value_width]
    decay_pre = terms[:, 2 * key_width + 2 * value_width : 3 * key_width + 2 * value_width]
    log_sigmoid = jnp.minimum(decay_pre, 0.0) - jnp.log1p(jnp.exp(-jnp.abs(decay_pre)))
    key_out[...] = keys
    value_out[...] = values
    keep = jnp.exp(log_sigmoid / gate_norm + log_decay[...])
    keep_out[...] = keep
    kept = query * keep
    columns = [kept[:, h * DK : (h + 1) * DK].T for h in range(heads)]
    for b in range(rows):
        for h in range(heads):
            attended[b : b + 1, h * DV : (h + 1) * DV] = jnp.sum(
                columns[h][:, b : b + 1] * state[b, h], axis=0, keepdims=True
            )
    for h in range(heads):
        lanes = slice(h * DK, (h + 1) * DK)
        outs = slice(h * DV, (h + 1) * DV)
        scores = jnp.sum(query[:, lanes] * keys[:, lanes], axis=1, keepdims=True)
        full = attended[:, outs] + scores * values[:, outs]
        scale = lax.rsqrt(jnp.mean(full * full, axis=1, keepdims=True) + eps)
        normed = full * scale * row(out_gain)
        mixed_out[:, outs] = (normed * jax.nn.silu(gate[:, outs])).astype(jnp.bfloat16)


def rows_kernel(count, *refs):
    blocks, (first, second, out) = refs[:count], refs[count:]
    left = jnp.concatenate([block[...] for block in blocks], axis=0)
    depth, model = second.shape
    start = lax.rem(lax.axis_index("kv"), 2) * depth if first.shape[0] > depth else 0
    kept = first[pl.ds(pl.multiple_of(start, depth), depth)] if first.shape[0] > depth else first[...]
    out[:, :model] = dot(left, kept).astype(jnp.bfloat16)
    out[:, model:] = dot(left, second[...]).astype(jnp.bfloat16)


def middle_kernel(n_even, n_odd, *refs):
    evens, odds = refs[:n_even], refs[n_even : n_even + n_odd]
    tokens, pair, mixer_gain, ffgate, sent = refs[n_even + n_odd :][:5]
    middle_out, own_out, other_out, *pieces = refs[n_even + n_odd + 5 :]
    me = lax.axis_index("kv")
    batch, model = tokens.shape
    half = ffgate.shape[1] // 2
    count = 2 * len(pieces)
    rows = batch // count
    even = sum(wide(ref[...]) for ref in evens)
    odd = sum(wide(ref[...]) for ref in odds)

    def pair_block(m):
        return pair[(m ^ 1) * rows : ((m ^ 1) + 1) * rows]

    def stream(stay, first, second):
        blocks = []
        for m in range(count):
            source = first if m % 2 == 0 else second
            blocks.append(wide(stay(m)) + source[m // 2 * rows : (m // 2 + 1) * rows])
        return wide(jnp.concatenate(blocks, axis=0).astype(jnp.bfloat16))

    own = stream(lambda m: block_of(tokens, me, m, rows), even[:, :model], odd[:, model:])
    other = stream(pair_block, even[:, model:], odd[:, :model])
    middle_out[...] = own.astype(jnp.bfloat16)
    own2 = (own * row(mixer_gain)).astype(jnp.bfloat16)
    other2 = (other * wide(pair[batch : batch + 1])).astype(jnp.bfloat16)
    own_out[...] = own2
    other_out[...] = other2
    squares = jnp.sum(own * own, axis=1, keepdims=True) + jnp.sum(other * other, axis=1, keepdims=True)
    kept = pl.ds(pl.multiple_of(lax.rem(me, 2) * half, half), half)
    gate = (dot(own2, ffgate[:, kept]) + dot(other2, sent[:, :half])).astype(jnp.bfloat16)
    size = 2 * rows
    for i, piece in enumerate(pieces):
        part = slice(i * size, (i + 1) * size)
        for j in range(half // LANES):
            piece[j * size : (j + 1) * size] = gate[part, j * LANES : (j + 1) * LANES]
        flat = jnp.broadcast_to(squares[part], (size, LANES)).T[:TILE]
        head = flat.astype(jnp.bfloat16)
        rest = (flat - wide(head)).astype(jnp.bfloat16)
        line = lax.broadcasted_iota(jnp.int32, flat.shape, 0)
        piece[-TILE:] = jnp.zeros((TILE, LANES), jnp.bfloat16)
        piece[-TILE:, :size] = jnp.where(line < TILE // 2, head, rest)


def upper_kernel(own2, other2, ffup, early, late, *pieces):
    half = ffup.shape[1] // 2
    first = half - late.shape[1]
    rows = own2.shape[0] // len(pieces)
    kept = pl.ds(pl.multiple_of(lax.rem(lax.axis_index("kv"), 2) * half, half), half)
    upper = dot(own2[...], ffup[:, kept])
    for columns, weight in ((slice(0, first), early[:, half:]), (slice(first, half), late[...])):
        part = (upper[:, columns] + dot(other2[...], weight)).astype(jnp.bfloat16)
        for i, piece in enumerate(pieces):
            piece[:, columns] = part[i * rows : (i + 1) * rows]


def hidden_kernel(count, *refs):
    gates, uppers, out = refs[:count], refs[count : 2 * count], refs[2 * count]
    half = out.shape[1]
    size = out.shape[0]
    terms = sum(wide(piece[...]) for piece in gates)
    upper = sum(wide(piece[...]) for piece in uppers)
    squares = terms[-TILE:, :size]
    squares = squares[:1] + squares[TILE // 2 : TILE // 2 + 1]
    inv = lax.rsqrt(jnp.broadcast_to(squares, (LANES, size)).T[:, :1] / D + eps)
    gate = [terms[j * size : (j + 1) * size] for j in range(half // LANES)]
    hidden = jax.nn.silu(jnp.concatenate(gate, axis=1) * inv) * (upper * inv)
    out[...] = hidden.astype(jnp.bfloat16)


def body(
    tokens,
    norm_gain,
    w_query,
    w_key,
    w_value,
    w_gate,
    w_decay,
    log_decay,
    state,
    out_gain,
    w_out,
    mixer_gain,
    w_ffgate,
    w_ffup,
    w_down,
):
    n_kv = lax.axis_size("kv")
    n_tp = lax.axis_size("tp")
    kv, tp, both = {"kv": n_kv}, {"tp": n_tp}, {"kv": n_kv, "tp": n_tp}
    me = lax.axis_index("kv")
    rows = state.shape[0]
    key_width = w_query.shape[1]
    value_width = w_value.shape[1]
    model = tokens.shape[1]
    half = w_ffgate.shape[1] // 2

    batch = tokens.shape[0]
    attn_weights = (w_query, w_key, w_value, w_gate, w_decay)
    total_width = sum(w.shape[1] for w in attn_weights) + LANES
    late = half * LATE // (6 * LANES) * LANES
    loaded = (tokens, norm_gain, mixer_gain) + attn_weights
    made = call(
        functools.partial(project_kernel, n_kv, rows),
        [shape((rows + (m == 1) * rows, total_width)) for m in range(n_kv - 1)]
        + [shape((model, half + half - late)), shape((model, late))]
        + [shape((half, model)), shape((batch + rows, model))],
        *in_hbm(*loaded, w_ffgate, w_ffup, w_down),
        specs=[HBM] * 11,
        out_specs=[VMEM] * (n_kv + 3),
        scratch=[pltpu.VMEM(w.shape, w.dtype) for w in loaded]
        + [pltpu.SemaphoreType.DMA((12,))],
    )
    pieces, (early_sent, late_sent, down_sent, pair_sent) = made[: n_kv - 1], made[n_kv - 1 :]
    order = order_of(SCATTER, range(1, n_kv - 1))
    came = {}
    came[1] = send_xor(pieces[1], kv, (1,))
    relayed = call(relay_kernel, shape((rows, total_width)), pieces[n_kv - 2], came[1])
    for m in [m for m in order if m != 1]:
        came[m] = send_xor(relayed if m == n_kv - 2 else pieces[m], kv, (m,))
    out_pair = send_xor(w_out, kv, (1,))
    early_pair = send_xor(early_sent, kv, (1,))
    pair = send_xor(pair_sent, kv, (1,))
    late_pair = send_xor(late_sent, kv, (1,))
    down_pair = send_xor(down_sent, kv, (1,))
    state_near, log_decay_near, out_gain_near = call(
        load_kernel,
        [pltpu.VMEM(x.shape, x.dtype) for x in (state, log_decay, out_gain)],
        *in_hbm(state, log_decay, out_gain),
        specs=[HBM] * 3,
        scratch=[pltpu.SemaphoreType.DMA((3,))],
    )

    mixed, keep, keys, values = call(
        functools.partial(attend_kernel, n_kv - 1, key_width),
        [shape((rows, value_width))]
        + [shape((rows, w), jnp.float32) for w in (key_width, key_width, value_width)],
        pieces[0],
        *[came[m] for m in order],
        log_decay_near,
        state_near,
        out_gain_near,
        scratch=[pltpu.VMEM((rows, value_width), jnp.float32)],
    )

    evens = list(range(2, n_kv, 2))
    blocks = {}
    for m in order_of(NEAR, evens):
        blocks[m] = send_xor(mixed, kv, (m,))
    new_state = call(
        functools.partial(update_kernel, STEPS),
        shape(state.shape, jnp.float32),
        state_near,
        keep,
        keys,
        values,
        out_specs=HBM,
        scratch=[
            pltpu.VMEM(state.shape, jnp.float32),
            pltpu.SemaphoreType.DMA((STEPS,)),
        ],
    )
    chip = call(
        functools.partial(rows_kernel, n_kv // 2),
        shape((n_kv // 2 * rows, 2 * model)),
        mixed,
        *[blocks[m] for m in evens],
        w_out,
        out_pair,
    )
    chip_core = send_xor(chip, tp, (1,))
    sent = (wide(chip) + wide(chip_core)).astype(jnp.bfloat16)
    even, odd = [chip, chip_core], []
    for m in range(0, n_tp, 2)[::-1]:
        odd.append(send_xor(sent, both, (1, m)))
        if m:
            even.append(send_xor(sent, both, (0, m)))

    middle, own2, other2, *gates = call(
        functools.partial(middle_kernel, len(even), len(odd)),
        [shape((batch, model))] * 3 + [shape((half // LANES * 2 * rows + TILE, LANES))] * (n_kv // 2),
        *even,
        *odd,
        tokens,
        pair,
        mixer_gain,
        w_ffgate,
        early_pair,
    )
    terms2 = [gates[0]]
    for m in order_of(FF_GATE, evens):
        terms2.append(send_xor(gates[m // 2], kv, (m,)))
    uppers = call(
        upper_kernel,
        [shape((2 * rows, half))] * (n_kv // 2),
        own2,
        other2,
        w_ffup,
        early_pair,
        late_pair,
    )
    terms2.append(uppers[0])
    for m in order_of(FF_UP, evens):
        terms2.append(send_xor(uppers[m // 2], kv, (m,)))
    hidden = call(functools.partial(hidden_kernel, n_kv // 2), shape((2 * rows, half)), *terms2)

    blocks = {}
    for m in order_of(HIDDEN, evens):
        blocks[m] = send_xor(hidden, kv, (m,))
    down = call(
        functools.partial(rows_kernel, n_kv // 2),
        shape((batch, 2 * model)),
        hidden,
        *[blocks[m] for m in evens],
        w_down,
        down_pair,
    )
    down = wide(down) + wide(send_xor(down, tp, (1,)))
    own, other = down[:, :model], down[:, model:].astype(jnp.bfloat16)
    sent = own.astype(jnp.bfloat16)
    crossed = 0.0
    for m in range(0, n_tp, 2)[::-1]:
        crossed = crossed + wide(send_xor(other, both, (1, m)))
        if m:
            own = own + wide(send_xor(sent, both, (0, m)))
    crossed = crossed.reshape(n_kv // 2, 2, rows, model)
    crossed = jnp.concatenate([crossed[:, 1:], crossed[:, :1]], axis=1).reshape(own.shape)
    result = (wide(middle) + own + crossed).astype(jnp.bfloat16)
    return (swap_blocks(result, me, n_kv), new_state)


def order_of(wanted, masks):
    if sorted(wanted) == sorted(masks):
        return list(wanted)
    return [m for m in masks if m == 1] + [m for m in masks if m != 1][::-1]


def solution(mesh):
    return jax.shard_map(
        body,
        mesh=mesh,
        in_specs=(
            P(None, "kv"),
            P("kv"),
            P("kv", "tp"),
            P("kv", "tp"),
            P("kv", "tp"),
            P("kv", "tp"),
            P("kv", "tp"),
            P("kv", "tp"),
            P("kv", "tp", None, None),
            P(),
            P("tp", "kv"),
            P("kv"),
            P("kv", "tp"),
            P("kv", "tp"),
            P("tp", "kv"),
        ),
        out_specs=(P(None, "kv"), P("kv", "tp", None, None)),
        check_vma=False,
    )
```

```python
import functools

import jax
import jax.numpy as jnp
from jax import lax
from jax.experimental import pallas as pl
from jax.experimental.pallas import tpu as pltpu
from jax.sharding import PartitionSpec as P


D = 2048
DK = 128
DV = 256
LANES = 128
TILE = 8
STEPS = 8
SCATTER = (1, 3, 4, 5, 6, 2)
NEAR = (6, 4, 2)
FF_GATE = (4, 6, 2)
FF_UP = (6, 4, 2)
LATE = 4
HIDDEN = (6, 4, 2)


eps = 1e-06
gate_norm = 16.0


def swap_blocks(array, me, count):
    rows = array.shape[0] // count
    half = 1
    while half < count:
        view = array.reshape(count // (2 * half), 2, half * rows, array.shape[1])
        flipped = jnp.concatenate([view[:, 1:], view[:, :1]], axis=1)
        array = jnp.where((me // half) % 2 == 1, flipped, view).reshape(array.shape)
        half *= 2
    return array


def send_xor(array, sizes, masks):
    if len(sizes) == 1:
        (axis,) = sizes
        pairs = [(i, i ^ masks[0]) for i in range(sizes[axis])]
        return lax.ppermute(array, axis, pairs)
    (first, outer), (second, inner) = sizes.items()
    pairs = [
        (i * inner + j, (i ^ masks[0]) * inner + (j ^ masks[1]))
        for i in range(outer)
        for j in range(inner)
    ]
    return lax.ppermute(array, (first, second), pairs)


def wide(array):
    return array.astype(jnp.float32)


def dot(left, right):
    return jnp.dot(left, right, preferred_element_type=jnp.float32)


def split_squares(squares):
    head = squares.astype(jnp.bfloat16)
    rest = (squares - head.astype(jnp.float32)).astype(jnp.bfloat16)
    lane = lax.broadcasted_iota(jnp.int32, (squares.shape[0], LANES), 1)
    return jnp.where(lane < LANES // 2, head, rest)


def joined_squares(block):
    return block[:, :1] + block[:, LANES // 2 : LANES // 2 + 1]


VMEM = pl.BlockSpec(memory_space=pltpu.VMEM)
HBM = pl.BlockSpec(memory_space=pltpu.HBM)


def call(kernel, outs, *args, specs=None, out_specs=None, scratch=(), grant=8 << 20):
    return pl.pallas_call(
        kernel,
        out_shape=outs,
        in_specs=specs or [VMEM] * len(args),
        out_specs=out_specs or jax.tree.map(lambda _: VMEM, outs),
        scratch_shapes=list(scratch),
        compiler_params=pltpu.CompilerParams(vmem_limit_bytes=grant),
    )(*args)


def in_hbm(*arrays):
    return [pltpu.with_memory_space_constraint(array, pltpu.HBM) for array in arrays]


def shape(dims, dtype=jnp.bfloat16):
    return jax.ShapeDtypeStruct(dims, dtype)


def row(ref):
    return wide(ref[...])[None]


def block_of(ref, me, m, rows):
    return ref[pl.ds(pl.multiple_of((me ^ m) * rows, rows), rows), :]


def place_of(m, count, rows):
    return (1, slice(rows, 2 * rows)) if m == count - 1 else (m, slice(0, rows))


def relay_kernel(piece, came, out):
    rows = piece.shape[0]
    terms = wide(piece[...]) + wide(came[rows:])
    out[:, :-LANES] = terms[:, :-LANES].astype(jnp.bfloat16)
    out[:, -LANES:] = split_squares(joined_squares(terms[:, -LANES:]))


def project_kernel(count, rows, *refs):
    loaded, (ffgate, ffup, down) = refs[:8], refs[8:11]
    pieces, (early_out, late_out, down_out, pair_out) = refs[11 : 10 + count], refs[10 + count : 14 + count]
    staged, sems = refs[14 + count : 22 + count], refs[22 + count]
    me = lax.axis_index("kv")
    other = 1 - lax.rem(me, 2)
    half = ffgate.shape[1] // 2
    start = pl.multiple_of(other * half, LANES)
    first = half - late_out.shape[1]
    loads = [pltpu.make_async_copy(w, s, sems.at[j]) for j, (w, s) in enumerate(zip(loaded, staged))]
    for load in loads:
        load.start()
    moves = [
        pltpu.make_async_copy(ffgate.at[:, pl.ds(start, half)], early_out.at[:, :half], sems.at[8]),
        pltpu.make_async_copy(ffup.at[:, pl.ds(start, first)], early_out.at[:, half:], sems.at[9]),
        pltpu.make_async_copy(ffup.at[:, pl.ds(start + first, half - first)], late_out, sems.at[10]),
        pltpu.make_async_copy(down.at[pl.ds(start, half)], down_out, sems.at[11]),
    ]
    for move in moves:
        move.start()
    tokens, norm_gain, mixer_gain = staged[:3]
    for load in loads[:3]:
        load.wait()
    mine = jnp.concatenate([block_of(tokens, me, m, rows) for m in range(count)], axis=0)
    total, model = tokens.shape
    share = total // 2
    first_rows = lax.rem(lax.axis_index("tp"), 2) == 0
    pair_out[:share] = jnp.where(first_rows, mine[:share], mine[share:])
    pair_out[share:] = jnp.broadcast_to(row(mixer_gain), (rows, model)).astype(jnp.bfloat16)
    mine = wide(mine)
    scaled = (mine * row(norm_gain)).astype(jnp.bfloat16)
    squares = split_squares(jnp.sum(mine * mine, axis=1, keepdims=True))
    at = 0
    for load, weight in zip(loads[3:], staged[3:]):
        load.wait()
        width = weight.shape[1]
        terms = dot(scaled, weight[...]).astype(jnp.bfloat16)
        for m in range(count):
            block, top = place_of(m, count, rows)
            pieces[block][top, at : at + width] = terms[m * rows : (m + 1) * rows]
        at += width
    for m in range(count):
        block, top = place_of(m, count, rows)
        pieces[block][top, at:] = squares[m * rows : (m + 1) * rows]
    for move in moves:
        move.wait()


def load_kernel(*refs):
    loads = [pltpu.make_async_copy(refs[j], refs[3 + j], refs[6].at[j]) for j in range(3)]
    for load in loads:
        load.start()
    for load in loads:
        load.wait()


def update_kernel(steps, state, keep, keys, values, out, fresh, sems):
    rows, heads = state.shape[:2]
    some = rows // steps
    keep_columns = [keep[:, h * DK : (h + 1) * DK].T for h in range(heads)]
    key_columns = [keys[:, h * DK : (h + 1) * DK].T for h in range(heads)]
    stores = []
    for i in range(steps):
        for b in range(i * some, (i + 1) * some):
            for h in range(heads):
                fresh[b, h] = (
                    keep_columns[h][:, b : b + 1] * state[b, h]
                    + key_columns[h][:, b : b + 1] * values[b : b + 1, h * DV : (h + 1) * DV]
                )
        part = pl.ds(i * some, some)
        stores.append(pltpu.make_async_copy(fresh.at[part], out.at[part], sems.at[i]))
        stores[-1].start()
    for store in stores:
        store.wait()


def attend_kernel(count, key_width, *refs):
    pieces, (log_decay, state, out_gain) = refs[:count], refs[count : count + 3]
    mixed_out, keep_out, key_out, value_out, attended = refs[count + 3 :]
    rows, heads = state.shape[:2]
    terms = wide(pieces[0][...])
    for piece in pieces[1:]:
        terms = terms + wide(piece[:rows])
    inv = lax.rsqrt(joined_squares(terms[:, -LANES:]) / D + eps)
    terms = terms * inv
    value_width = heads * DV
    query = terms[:, :key_width] * DK ** (-0.5)
    keys = terms[:, key_width : 2 * key_width]
    values = terms[:, 2 * key_width : 2 * key_width + value_width]
    gate = terms[:, 2 * key_width + value_width : 2 * key_width + 2 * value_width]
    decay_pre = terms[:, 2 * key_width + 2 * value_width : 3 * key_width + 2 * value_width]
    log_sigmoid = jnp.minimum(decay_pre, 0.0) - jnp.log1p(jnp.exp(-jnp.abs(decay_pre)))
    key_out[...] = keys
    value_out[...] = values
    keep = jnp.exp(log_sigmoid / gate_norm + log_decay[...])
    keep_out[...] = keep
    kept = query * keep
    columns = [kept[:, h * DK : (h + 1) * DK].T for h in range(heads)]
    for b in range(rows):
        for h in range(heads):
            attended[b : b + 1, h * DV : (h + 1) * DV] = jnp.sum(
                columns[h][:, b : b + 1] * state[b, h], axis=0, keepdims=True
            )
    for h in range(heads):
        lanes = slice(h * DK, (h + 1) * DK)
        outs = slice(h * DV, (h + 1) * DV)
        scores = jnp.sum(query[:, lanes] * keys[:, lanes], axis=1, keepdims=True)
        full = attended[:, outs] + scores * values[:, outs]
        scale = lax.rsqrt(jnp.mean(full * full, axis=1, keepdims=True) + eps)
        normed = full * scale * row(out_gain)
        mixed_out[:, outs] = (normed * jax.nn.silu(gate[:, outs])).astype(jnp.bfloat16)


def rows_kernel(count, *refs):
    blocks, (first, second, out) = refs[:count], refs[count:]
    left = jnp.concatenate([block[...] for block in blocks], axis=0)
    depth, model = second.shape
    start = lax.rem(lax.axis_index("kv"), 2) * depth if first.shape[0] > depth else 0
    kept = first[pl.ds(pl.multiple_of(start, depth), depth)] if first.shape[0] > depth else first[...]
    out[:, :model] = dot(left, kept).astype(jnp.bfloat16)
    out[:, model:] = dot(left, second[...]).astype(jnp.bfloat16)


def middle_kernel(n_even, n_odd, *refs):
    evens, odds = refs[:n_even], refs[n_even : n_even + n_odd]
    tokens, pair, pair_core, mixer_gain, ffgate, sent = refs[n_even + n_odd :][:6]
    middle_out, own_out, other_out, *pieces = refs[n_even + n_odd + 6 :]
    me = lax.axis_index("kv")
    batch, model = tokens.shape
    half = ffgate.shape[1] // 2
    count = 2 * len(pieces)
    rows = batch // count
    even = sum(wide(ref[...]) for ref in evens)
    odd = sum(wide(ref[...]) for ref in odds)

    first_rows = lax.rem(lax.axis_index("tp"), 2) == 0

    def pair_block(m):
        at = (m ^ 1) * rows
        low = at < batch // 2
        part = slice(at % (batch // 2), at % (batch // 2) + rows)
        return jnp.where(first_rows == low, pair[part], pair_core[part])

    def stream(stay, first, second):
        blocks = []
        for m in range(count):
            source = first if m % 2 == 0 else second
            blocks.append(wide(stay(m)) + source[m // 2 * rows : (m // 2 + 1) * rows])
        return wide(jnp.concatenate(blocks, axis=0).astype(jnp.bfloat16))

    own = stream(lambda m: block_of(tokens, me, m, rows), even[:, :model], odd[:, model:])
    other = stream(pair_block, even[:, model:], odd[:, :model])
    middle_out[...] = own.astype(jnp.bfloat16)
    own2 = (own * row(mixer_gain)).astype(jnp.bfloat16)
    other2 = (other * wide(pair[batch // 2 : batch // 2 + 1])).astype(jnp.bfloat16)
    own_out[...] = own2
    other_out[...] = other2
    squares = jnp.sum(own * own, axis=1, keepdims=True) + jnp.sum(other * other, axis=1, keepdims=True)
    kept = pl.ds(pl.multiple_of(lax.rem(me, 2) * half, half), half)
    gate = (dot(own2, ffgate[:, kept]) + dot(other2, sent[:, :half])).astype(jnp.bfloat16)
    size = 2 * rows
    for i, piece in enumerate(pieces):
        part = slice(i * size, (i + 1) * size)
        for j in range(half // LANES):
            piece[j * size : (j + 1) * size] = gate[part, j * LANES : (j + 1) * LANES]
        flat = jnp.broadcast_to(squares[part], (size, LANES)).T[:TILE]
        head = flat.astype(jnp.bfloat16)
        rest = (flat - wide(head)).astype(jnp.bfloat16)
        line = lax.broadcasted_iota(jnp.int32, flat.shape, 0)
        piece[-TILE:] = jnp.zeros((TILE, LANES), jnp.bfloat16)
        piece[-TILE:, :size] = jnp.where(line < TILE // 2, head, rest)


def upper_kernel(own2, other2, ffup, early, late, *pieces):
    half = ffup.shape[1] // 2
    first = half - late.shape[1]
    rows = own2.shape[0] // len(pieces)
    kept = pl.ds(pl.multiple_of(lax.rem(lax.axis_index("kv"), 2) * half, half), half)
    upper = dot(own2[...], ffup[:, kept])
    for columns, weight in ((slice(0, first), early[:, half:]), (slice(first, half), late[...])):
        part = (upper[:, columns] + dot(other2[...], weight)).astype(jnp.bfloat16)
        for i, piece in enumerate(pieces):
            piece[:, columns] = part[i * rows : (i + 1) * rows]


def hidden_kernel(count, *refs):
    gates, uppers, out = refs[:count], refs[count : 2 * count], refs[2 * count]
    half = out.shape[1]
    size = out.shape[0]
    terms = sum(wide(piece[...]) for piece in gates)
    upper = sum(wide(piece[...]) for piece in uppers)
    squares = terms[-TILE:, :size]
    squares = squares[:1] + squares[TILE // 2 : TILE // 2 + 1]
    inv = lax.rsqrt(jnp.broadcast_to(squares, (LANES, size)).T[:, :1] / D + eps)
    gate = [terms[j * size : (j + 1) * size] for j in range(half // LANES)]
    hidden = jax.nn.silu(jnp.concatenate(gate, axis=1) * inv) * (upper * inv)
    out[...] = hidden.astype(jnp.bfloat16)


def body(
    tokens,
    norm_gain,
    w_query,
    w_key,
    w_value,
    w_gate,
    w_decay,
    log_decay,
    state,
    out_gain,
    w_out,
    mixer_gain,
    w_ffgate,
    w_ffup,
    w_down,
):
    n_kv = lax.axis_size("kv")
    n_tp = lax.axis_size("tp")
    kv, tp, both = {"kv": n_kv}, {"tp": n_tp}, {"kv": n_kv, "tp": n_tp}
    me = lax.axis_index("kv")
    rows = state.shape[0]
    key_width = w_query.shape[1]
    value_width = w_value.shape[1]
    model = tokens.shape[1]
    half = w_ffgate.shape[1] // 2

    batch = tokens.shape[0]
    attn_weights = (w_query, w_key, w_value, w_gate, w_decay)
    total_width = sum(w.shape[1] for w in attn_weights) + LANES
    late = half * LATE // (6 * LANES) * LANES
    loaded = (tokens, norm_gain, mixer_gain) + attn_weights
    made = call(
        functools.partial(project_kernel, n_kv, rows),
        [shape((rows + (m == 1) * rows, total_width)) for m in range(n_kv - 1)]
        + [shape((model, half + half - late)), shape((model, late))]
        + [shape((half, model)), shape((batch // 2 + rows, model))],
        *in_hbm(*loaded, w_ffgate, w_ffup, w_down),
        specs=[HBM] * 11,
        out_specs=[VMEM] * (n_kv + 3),
        scratch=[pltpu.VMEM(w.shape, w.dtype) for w in loaded]
        + [pltpu.SemaphoreType.DMA((12,))],
    )
    pieces, (early_sent, late_sent, down_sent, pair_sent) = made[: n_kv - 1], made[n_kv - 1 :]
    order = order_of(SCATTER, range(1, n_kv - 1))
    came = {}
    came[1] = send_xor(pieces[1], kv, (1,))
    relayed = call(relay_kernel, shape((rows, total_width)), pieces[n_kv - 2], came[1])
    for m in [m for m in order if m != 1]:
        came[m] = send_xor(relayed if m == n_kv - 2 else pieces[m], kv, (m,))
    out_pair = send_xor(w_out, kv, (1,))
    early_pair = send_xor(early_sent, kv, (1,))
    pair = send_xor(pair_sent, kv, (1,))
    pair_core = send_xor(pair, tp, (1,))
    late_pair = send_xor(late_sent, kv, (1,))
    down_pair = send_xor(down_sent, kv, (1,))
    state_near, log_decay_near, out_gain_near = call(
        load_kernel,
        [pltpu.VMEM(x.shape, x.dtype) for x in (state, log_decay, out_gain)],
        *in_hbm(state, log_decay, out_gain),
        specs=[HBM] * 3,
        scratch=[pltpu.SemaphoreType.DMA((3,))],
    )

    mixed, keep, keys, values = call(
        functools.partial(attend_kernel, n_kv - 1, key_width),
        [shape((rows, value_width))]
        + [shape((rows, w), jnp.float32) for w in (key_width, key_width, value_width)],
        pieces[0],
        *[came[m] for m in order],
        log_decay_near,
        state_near,
        out_gain_near,
        scratch=[pltpu.VMEM((rows, value_width), jnp.float32)],
    )

    evens = list(range(2, n_kv, 2))
    blocks = {}
    for m in order_of(NEAR, evens):
        blocks[m] = send_xor(mixed, kv, (m,))
    new_state = call(
        functools.partial(update_kernel, STEPS),
        shape(state.shape, jnp.float32),
        state_near,
        keep,
        keys,
        values,
        out_specs=HBM,
        scratch=[
            pltpu.VMEM(state.shape, jnp.float32),
            pltpu.SemaphoreType.DMA((STEPS,)),
        ],
    )
    chip = call(
        functools.partial(rows_kernel, n_kv // 2),
        shape((n_kv // 2 * rows, 2 * model)),
        mixed,
        *[blocks[m] for m in evens],
        w_out,
        out_pair,
    )
    chip_core = send_xor(chip, tp, (1,))
    sent = (wide(chip) + wide(chip_core)).astype(jnp.bfloat16)
    even, odd = [chip, chip_core], []
    for m in range(0, n_tp, 2)[::-1]:
        odd.append(send_xor(sent, both, (1, m)))
        if m:
            even.append(send_xor(sent, both, (0, m)))

    middle, own2, other2, *gates = call(
        functools.partial(middle_kernel, len(even), len(odd)),
        [shape((batch, model))] * 3 + [shape((half // LANES * 2 * rows + TILE, LANES))] * (n_kv // 2),
        *even,
        *odd,
        tokens,
        pair,
        pair_core,
        mixer_gain,
        w_ffgate,
        early_pair,
    )
    terms2 = [gates[0]]
    for m in order_of(FF_GATE, evens):
        terms2.append(send_xor(gates[m // 2], kv, (m,)))
    uppers = call(
        upper_kernel,
        [shape((2 * rows, half))] * (n_kv // 2),
        own2,
        other2,
        w_ffup,
        early_pair,
        late_pair,
    )
    terms2.append(uppers[0])
    for m in order_of(FF_UP, evens):
        terms2.append(send_xor(uppers[m // 2], kv, (m,)))
    hidden = call(functools.partial(hidden_kernel, n_kv // 2), shape((2 * rows, half)), *terms2)

    blocks = {}
    for m in order_of(HIDDEN, evens):
        blocks[m] = send_xor(hidden, kv, (m,))
    down = call(
        functools.partial(rows_kernel, n_kv // 2),
        shape((batch, 2 * model)),
        hidden,
        *[blocks[m] for m in evens],
        w_down,
        down_pair,
    )
    down = wide(down) + wide(send_xor(down, tp, (1,)))
    own, other = down[:, :model], down[:, model:].astype(jnp.bfloat16)
    sent = own.astype(jnp.bfloat16)
    crossed = 0.0
    for m in range(0, n_tp, 2)[::-1]:
        crossed = crossed + wide(send_xor(other, both, (1, m)))
        if m:
            own = own + wide(send_xor(sent, both, (0, m)))
    crossed = crossed.reshape(n_kv // 2, 2, rows, model)
    crossed = jnp.concatenate([crossed[:, 1:], crossed[:, :1]], axis=1).reshape(own.shape)
    result = (wide(middle) + own + crossed).astype(jnp.bfloat16)
    return (swap_blocks(result, me, n_kv), new_state)


def order_of(wanted, masks):
    if sorted(wanted) == sorted(masks):
        return list(wanted)
    return [m for m in masks if m == 1] + [m for m in masks if m != 1][::-1]


def solution(mesh):
    return jax.shard_map(
        body,
        mesh=mesh,
        in_specs=(
            P(None, "kv"),
            P("kv"),
            P("kv", "tp"),
            P("kv", "tp"),
            P("kv", "tp"),
            P("kv", "tp"),
            P("kv", "tp"),
            P("kv", "tp"),
            P("kv", "tp", None, None),
            P(),
            P("tp", "kv"),
            P("kv"),
            P("kv", "tp"),
            P("kv", "tp"),
            P("tp", "kv"),
        ),
        out_specs=(P(None, "kv"), P("kv", "tp", None, None)),
        check_vma=False,
    )
```
